32 devices in a mesh: sp: 16 (over z, y, x), tp: 2 (over core).
Axes of the slice: x: 2, y: 2, z: 4, core: 2. Of those that a mesh axis runs over, the one named last changes fastest.
Arguments:
- queries: bfloat16 [4096, 8, 128], P('sp', 'tp'), may hold values from -6 to 6
- keys: bfloat16 [4096, 2, 128], P('sp'), may hold values from -6 to 6
- values: bfloat16 [4096, 2, 128], P('sp'), may hold values from -6 to 6
- documents: int32 [4096], P('sp'), may hold values from 0 to 3, never falling along the last dimension, each value on 1 to 2304 neighbouring positions
- query_gain: float32 [128], replicated, may hold values from 0.25 to 4
- key_gain: float32 [128], replicated, may hold values from 0.25 to 4
- out_weight: bfloat16 [1024, 2048], P('tp'), may hold values from -0.1875 to 0.1875
- residual: bfloat16 [4096, 2048], P('sp'), may hold values from -6 to 6
- norm_gain: float32 [2048], replicated, may hold values from 0.1 to 1.9
- up_weight: bfloat16 [2048, 6144], P('sp', 'tp'), may hold values from -0.125 to 0.125
- down_weight: bfloat16 [2048, 6144], P('sp', 'tp'), may hold values from -0.078125 to 0.078125
Outputs:
- layer_out: bfloat16 [4096, 2048], P(('sp', 'tp'))
The draws below stay inside these ranges and needn't reach their ends.
Inputs may be any that keep to these rules, and one draw needn't show every extreme that they name: `documents`: document numbers never fall along the sequence; one document covers exactly (9) * 256 positions.
All inputs are finite; a program needn't handle non-finite values.
Results may differ from the reference program's by a relative error of at most 0.017.
Values may be sent and summed in bfloat16 or wider, within the bound.
No kernel may reach another device: no remote copies, remote signals or barrier semaphores. Data moves between devices by JAX's collectives and lax.ppermute only.
A program may use at most 128 MiB of HBM per device.

```python
import math
import jax
import jax.numpy as jnp
import numpy as np
from jax import lax

D = 2048
QUERY_HEADS = 8
KEY_VALUE_HEADS = 2
HEAD_SIZE = 128
FF = 6144
GRID = 64
TOKENS_PER_SHARD = 256
PACKED_TOKENS = 4096
N_SP = 16
N_TP = 2


def group_shared_keys(key):
    return jax.random.truncated_normal(jax.random.fold_in(key, 31), -6.0, 6.0, (PACKED_TOKENS, KEY_VALUE_HEADS, HEAD_SIZE), jnp.float32)


def draw_keys(key, part):
    return group_shared_keys(key).astype(jnp.bfloat16)


def draw_queries(key, part):
    fresh = jax.random.truncated_normal(jax.random.fold_in(key, 37), -6.0, 6.0, (PACKED_TOKENS, QUERY_HEADS, HEAD_SIZE), jnp.float32)
    return fresh.astype(jnp.bfloat16)


def draw_query_gain(key, part):
    return 1.0 + 0.18 * jax.random.truncated_normal(jax.random.fold_in(key, 43), -4.0, 4.0, (HEAD_SIZE,), jnp.float32)


def draw_key_gain(key, part):
    return 1.0 + 0.18 * jax.random.truncated_normal(jax.random.fold_in(key, 53), -4.0, 4.0, (HEAD_SIZE,), jnp.float32)


def level_of(own_key, shape, shards, least, high):
    factor_of = 1.0
    for axis_at, blocks in shards:
        steps = jax.random.uniform(jax.random.fold_in(jax.random.fold_in(own_key, 6), axis_at), (blocks,), jnp.float32, least / len(shards), high / len(shards))
        factor_of = factor_of * jnp.repeat(jnp.exp(steps), shape[axis_at] // blocks).reshape((-1,) + (1,) * (len(shape) - 1 - axis_at))
    return factor_of


def profile(number_of, total, bound, slope):
    weights = [(1 << 20) // math.isqrt(standing ** slope) + 1 for standing in range(2, number_of + 1)]
    surplus, holding = total - bound - (number_of - 1), [1] * (number_of - 1)
    while surplus > 0:
        candidates = [i for i in range(number_of - 1) if holding[i] < bound]
        mass, budget = sum([weights[i] for i in candidates]), surplus
        for i in candidates:
            addition = min(bound - holding[i], max(1, budget * weights[i] // mass), surplus)
            holding[i] = holding[i] + addition
            surplus = surplus - addition
    return np.array([bound] + holding)


def uneven_parts(key, amount, total, most, lean):
    if amount == 2:
        one = jax.random.randint(key, (), max(1, total - most), min(most, total - 1) + 1)
        return jnp.stack([one, total - one])
    lengths = jnp.asarray(profile(amount, total, most, lean), jnp.int32)
    twos = (amount - 1) // 2
    source_of, taker = lengths[1:1 + 2 * twos:2], lengths[2:2 + 2 * twos:2]
    slack = jnp.minimum(source_of - 1, most - taker)
    shifted = jax.random.randint(jax.random.fold_in(key, 1), (twos,), 0, 1 << 20) % (slack + 1)
    lengths = lengths.at[1:1 + 2 * twos:2].set(source_of - shifted).at[2:2 + 2 * twos:2].set(taker + shifted)
    return lengths[jax.random.permutation(jax.random.fold_in(key, 2), amount)]


def scatter_about(rng, shape, scale, limit, split=(), kind=jnp.bfloat16):
    drawn = jax.random.normal(rng, shape, jnp.float32) * scale
    if len(split) > 0:
        drawn = level_of(rng, shape, split, -0.22, 0.18) * drawn
    return jnp.clip(drawn, min=-limit, max=limit).astype(kind)


def setup_inputs(seed: int = 0) -> dict:
    key_of = jax.random.split(jax.random.key(seed), 12)
    return {
        "queries": draw_queries(jax.random.fold_in(key_of[11], 71), 0),
        "keys": draw_keys(jax.random.fold_in(key_of[11], 71), 0),
        "values": scatter_about(key_of[2], (PACKED_TOKENS, KEY_VALUE_HEADS, HEAD_SIZE), 1.0, 6.0, ((0, 16),)),
        "documents": jnp.searchsorted(jnp.cumsum(uneven_parts(key_of[3], N_SP // 4, PACKED_TOKENS, (N_SP // 2 + 1) * TOKENS_PER_SHARD, 0)), jnp.arange(PACKED_TOKENS), side="right").astype(jnp.int32),
        "query_gain": draw_query_gain(jax.random.fold_in(key_of[11], 71), 0),
        "key_gain": draw_key_gain(jax.random.fold_in(key_of[11], 71), 0),
        "out_weight": scatter_about(key_of[6], (QUERY_HEADS * HEAD_SIZE, D), (QUERY_HEADS * HEAD_SIZE) ** -0.5, 0.1875, ((0, 2),)),
        "residual": scatter_about(key_of[7], (PACKED_TOKENS, D), 1.0, 6.0, ((0, 16),)),
        "norm_gain": jnp.clip(1.0 + 0.18 * jax.random.normal(key_of[8], (D,), jnp.float32), 0.1, 1.9),
        "up_weight": scatter_about(key_of[9], (D, FF), D ** -0.5, 0.125, ((0, 16), (1, 2))),
        "down_weight": scatter_about(key_of[10], (D, FF), FF ** -0.5, 0.078125, ((0, 16), (1, 2))),
    }


EPS = 1e-06
THETA = 10000.0

def head_norm(block, gain):
    return block * lax.rsqrt(lax.optimization_barrier(jnp.mean(block * block, axis=-1, keepdims=True)) + EPS) * gain

def rotate(block, positions):
    head_width = block.shape[-1]
    pair_count = head_width // 4
    inverse = THETA ** (-jnp.arange(pair_count, dtype=jnp.float32) / pair_count)
    grid_row = (positions // GRID).astype(jnp.float32)[:, None] * inverse
    grid_col = (positions % GRID).astype(jnp.float32)[:, None] * inverse
    angles = jnp.concatenate([grid_row, grid_row, grid_col, grid_col], axis=-1)
    cosine = jnp.cos(angles)[:, None, :]
    sine_table = jnp.sin(angles)[:, None, :]
    turned = jnp.concatenate([-block[..., pair_count:2 * pair_count], block[..., 0:pair_count], -block[..., 3 * pair_count:], block[..., 2 * pair_count:3 * pair_count]], axis=-1)
    return block * cosine + turned * sine_table

def channel_norm(rows_in, gain):
    widened = rows_in.astype(jnp.float32)
    return (widened * lax.rsqrt(lax.optimization_barrier(jnp.mean(widened * widened, axis=-1, keepdims=True)) + EPS) * gain).astype(jnp.bfloat16)

def rounded(value):
    return lax.optimization_barrier(value.astype(jnp.bfloat16)).astype(jnp.float32)

def reference(queries, keys, values, documents, query_gain, key_gain, out_weight, residual, norm_gain, up_weight, down_weight):
    positions = jnp.arange(PACKED_TOKENS, dtype=jnp.int32)
    rotated_query = rotate(head_norm(queries.astype(jnp.float32), query_gain), positions).astype(jnp.bfloat16)
    key_rot = rotate(head_norm(keys.astype(jnp.float32), key_gain), positions).astype(jnp.bfloat16)
    query_group_count = QUERY_HEADS // KEY_VALUE_HEADS
    key_wide = key_rot.astype(jnp.float32)
    value_wide = values.astype(jnp.float32)
    query_tiles = rotated_query.reshape(N_SP, TOKENS_PER_SHARD, KEY_VALUE_HEADS, query_group_count, HEAD_SIZE)
    doc_blocks = documents.reshape(N_SP, TOKENS_PER_SHARD)
    scale = HEAD_SIZE ** (-0.5)

    def attend(item):
        query_block, doc_block = item
        scores = jnp.einsum('qgrd,kgd->grqk', query_block.astype(jnp.float32), key_wide) * scale
        allowed = (doc_block[:, None] == documents[None, :])[None, None]
        scores = jnp.where(allowed, scores, -1e+30)
        peak = lax.optimization_barrier(jnp.max(scores, axis=-1, keepdims=True))
        probs = jnp.where(allowed, jnp.exp(scores - peak), 0.0)
        denom = lax.optimization_barrier(jnp.sum(probs, axis=-1))
        summed = jnp.einsum('grqk,kgd->qgrd', rounded(probs), value_wide)
        return (summed / jnp.transpose(denom, (2, 0, 1))[..., None]).astype(jnp.bfloat16)
    attn = lax.map(attend, (query_tiles, doc_blocks)).reshape(PACKED_TOKENS, QUERY_HEADS * HEAD_SIZE)
    span = QUERY_HEADS * HEAD_SIZE // N_TP
    branch = jnp.zeros((PACKED_TOKENS, D), jnp.float32)
    for index in range(N_TP):
        partial_term = jnp.dot(attn[:, index * span:(index + 1) * span], out_weight[index * span:(index + 1) * span], preferred_element_type=jnp.float32)
        branch = branch + rounded(partial_term)
    mid = (residual.astype(jnp.float32) + branch).astype(jnp.bfloat16)
    normed = channel_norm(mid, norm_gain)
    hidden_span = FF // N_TP
    mixer = jnp.zeros((PACKED_TOKENS, D), jnp.float32)
    for index in range(N_TP):
        raised = jnp.dot(normed, up_weight[:, index * hidden_span:(index + 1) * hidden_span], preferred_element_type=jnp.float32)
        hidden = jnp.square(jax.nn.relu(raised)).astype(jnp.bfloat16)
        partial_term = lax.dot_general(hidden, down_weight[:, index * hidden_span:(index + 1) * hidden_span], (((1,), (1,)), ((), ())), preferred_element_type=jnp.float32)
        mixer = mixer + rounded(partial_term)
    return (mid.astype(jnp.float32) + mixer).astype(jnp.bfloat16)
```

```python
import functools

import jax
import jax.numpy as jnp
from jax import lax
from jax.experimental import pallas as pl
from jax.experimental.pallas import tpu as pltpu
from jax.sharding import PartitionSpec as P

QUERY_HEADS = 8
GRID = 64
EPS = 1e-06
THETA = 10000.0
LANES = 128
DOC_ROWS = 16
LOG2E = 1.4426950408889634
VMEM = pl.BlockSpec(memory_space=pltpu.VMEM)
BF16, F32 = jnp.bfloat16, jnp.float32


def call(kernel, outs, args, scratch=(), flops=0, name=None):
    result = pl.pallas_call(
        kernel,
        out_shape=outs,
        in_specs=[VMEM] * len(args),
        out_specs=jax.tree.map(lambda _: VMEM, outs),
        scratch_shapes=list(scratch),
        compiler_params=pltpu.CompilerParams(vmem_limit_bytes=48 * 1024 * 1024),
        cost_estimate=pl.CostEstimate(flops=flops, bytes_accessed=0, transcendentals=0),
        name=name,
    )(*args)
    return list(result) if isinstance(outs, list) else result


def shape(dims, dtype=BF16):
    return jax.ShapeDtypeStruct(dims, dtype)


def ring_place(plane, planes):
    return jnp.where(plane % 2 == 1, (plane + 1) // 2, jnp.where(plane == 0, 0, planes - plane // 2))


def ring_plane(at, planes):
    return jnp.where(at <= planes // 2, jnp.maximum(2 * at - 1, 0), 2 * (planes - at))


def ring_order(planes):
    return [0] + list(range(1, planes, 2)) + list(range((planes - 1) // 2 * 2, 0, -2))


def plane_width(n_sp, columns):
    width = 1
    while (4 * width * width <= n_sp) and n_sp % (2 * width) == 0 and columns % (2 * width * LANES) == 0:
        width *= 2
    return width


def rope_tables(base, rows, head):
    quarter = head // 4
    lane = lax.broadcasted_iota(jnp.int32, (rows, head), 1)
    position = base + lax.broadcasted_iota(jnp.int32, (rows, head), 0)
    where = jnp.where(lane < 2 * quarter, position // GRID, position % GRID).astype(F32)
    step = (lane % quarter).astype(F32) / quarter
    angle = where * jnp.exp(step * (-jnp.log(jnp.float32(THETA))))
    first = lane % (2 * quarter) < quarter
    return jnp.cos(angle), jnp.sin(angle), first


def norm_rope(block, gain, tables):
    cosine, sine, first = tables
    head = block.shape[-1]
    block = block.astype(F32)
    block = block * lax.rsqrt(jnp.mean(block * block, axis=-1, keepdims=True) + EPS) * gain
    turned = jnp.where(first, -pltpu.roll(block, head - head // 4, 1), pltpu.roll(block, head // 4, 1))
    return (block * cosine + turned * sine).astype(BF16)


def key_kernel(key_ref, value_ref, doc_ref, gain_ref, out_ref):
    rows, head = key_ref.shape
    tables = rope_tables(lax.axis_index("sp") * rows, rows, head)
    out_ref[0:rows, 0:head] = norm_rope(key_ref[...], gain_ref[...], tables)
    out_ref[0:rows, head:] = value_ref[...]
    docs = doc_ref[...].astype(F32)
    out_ref[rows:, :] = jnp.broadcast_to(docs, (DOC_ROWS, rows)).astype(BF16)


def query_kernel(heads, query_ref, gain_ref, out_ref):
    rows = query_ref.shape[0]
    head = query_ref.shape[1] // heads
    tables = rope_tables(lax.axis_index("sp") * rows, rows, head)
    for h in range(heads):
        cols = slice(h * head, (h + 1) * head)
        out_ref[:, cols] = norm_rope(query_ref[:, cols], gain_ref[...], tables)


def attend_kernel(heads, n_tp, blocks, query_ref, doc_ref, out_weight_ref, *refs):
    kv_refs = refs[: -(n_tp + 4)]
    out_refs = refs[-(n_tp + 4) : -4]
    peak_ref, denom_ref, sum_ref, attn_ref = refs[-4:]
    rows = query_ref.shape[0]
    head = query_ref.shape[1] // heads
    height = rows + DOC_ROWS
    scale = head ** (-0.5) * LOG2E
    peak_ref[...] = jnp.full(peak_ref.shape, -1e30, F32)
    sum_ref[...] = jnp.zeros(sum_ref.shape, F32)
    denom_ref[...] = jnp.zeros(denom_ref.shape, F32)
    own = doc_ref[...].astype(F32)
    first_doc, last_doc = jnp.min(own), jnp.max(own)

    def block(kv_ref, at):
        docs = kv_ref[pl.ds(at + rows, DOC_ROWS), :].astype(F32)[0:1, :]

        @pl.when(jnp.logical_and(jnp.min(docs) <= last_doc, jnp.max(docs) >= first_doc))
        def _():
            allowed = own == docs
            keys = kv_ref[pl.ds(at, rows), 0:head]
            vals = kv_ref[pl.ds(at, rows), head:]
            for h in range(heads):
                s = lax.dot_general(
                    query_ref[:, h * head : (h + 1) * head],
                    keys,
                    (((1,), (1,)), ((), ())),
                    preferred_element_type=F32,
                )
                s = jnp.where(allowed, s * scale, -1e30)
                old = peak_ref[h]
                new = jnp.maximum(old, jnp.max(s, axis=-1, keepdims=True))
                peak_ref[h] = new
                p = jnp.where(allowed, jnp.exp2(s - new), 0.0)
                keep = jnp.exp2(old - new)
                denom_ref[h] = denom_ref[h] * keep + jnp.sum(p, axis=-1, keepdims=True)
                sum_ref[h] = sum_ref[h] * keep + jnp.dot(
                    p.astype(BF16), vals, preferred_element_type=F32
                )

    for kv_ref in kv_refs:

        @pl.loop(0, blocks)
        def _(i):
            block(kv_ref, pl.multiple_of(i * height, DOC_ROWS))

    for h in range(heads):
        attn_ref[:, h * head : (h + 1) * head] = (sum_ref[h] / denom_ref[h]).astype(BF16)
    share = rows // n_tp
    for j, out_ref in enumerate(out_refs):
        at = lax.rem(lax.axis_index("tp") + j, n_tp) * share
        out_ref[...] = jnp.dot(
            attn_ref[pl.ds(pl.multiple_of(at, share), share), :],
            out_weight_ref[...],
            preferred_element_type=F32,
        ).astype(BF16)


def mid_kernel(n_tp, residual_ref, gain_ref, *refs):
    part_refs, (mid_ref, normed_ref) = refs[:n_tp], refs[n_tp:]
    share = mid_ref.shape[0]
    at = pl.multiple_of(lax.axis_index("tp") * share, share)
    branch = part_refs[0][...].astype(F32)
    for part_ref in part_refs[1:]:
        branch = branch + part_ref[...].astype(F32)
    mid = (residual_ref[pl.ds(at, share), :].astype(F32) + branch).astype(BF16)
    mid_ref[...] = mid
    mid = mid.astype(F32)
    scale = lax.rsqrt(jnp.mean(mid * mid, axis=-1, keepdims=True) + EPS)
    normed_ref[...] = (mid * scale * gain_ref[...]).astype(BF16)


def up_kernel(pieces, planes, width, *refs):
    piece_refs, w_refs = refs[:pieces], refs[pieces:-3]
    out_ref, rows_ref, weight_ref = refs[-3:]
    share = piece_refs[0].shape[0]
    place = lax.rem(lax.axis_index("sp"), width)
    ring_at = ring_place(lax.div(lax.axis_index("sp"), width), planes)
    for n, piece_ref in enumerate(piece_refs):
        rows_ref[n * share : (n + 1) * share, :] = piece_ref[...]
    per_plane = len(w_refs) // planes
    for i in range(planes):
        plane = ring_plane(lax.rem(ring_at - i + planes, planes), planes)
        k = 0
        for w_ref in w_refs[i * per_plane : (i + 1) * per_plane]:
            for n in range(w_ref.shape[0]):
                weight_ref[plane * width + jnp.bitwise_xor(place, k)] = w_ref[n]
                k += 1
    weight = weight_ref[...].reshape(-1, weight_ref.shape[-1])
    tall = min(256, rows_ref.shape[0])

    @pl.loop(0, rows_ref.shape[0] // tall)
    def _(n):
        at = pl.ds(pl.multiple_of(n * tall, tall), tall)
        raised = jnp.dot(rows_ref[at, :], weight, preferred_element_type=F32)
        raised = jnp.maximum(raised, 0.0)
        out_ref[at, :] = (raised * raised).astype(BF16)


def sort_kernel(width, *refs):
    in_refs, out_refs = refs[:width], refs[width:]
    place = lax.rem(lax.axis_index("sp"), width)
    each = width // len(out_refs)
    for k, in_ref in enumerate(in_refs):
        to = jnp.bitwise_xor(place, k)
        for h, out_ref in enumerate(out_refs):

            @pl.when(lax.div(to, each) == h)
            def _():
                out_ref[lax.rem(to, each)] = in_ref[...]


def down_kernel(n_tp, hidden_ref, *refs):
    w_refs, out_refs = refs[:-n_tp], refs[-n_tp:]
    tall = out_refs[0].shape[0]
    for j, out_ref in enumerate(out_refs):
        at = 0
        for w_ref in w_refs:
            weight = w_ref[...].reshape(-1, w_ref.shape[-1])
            out_ref[:, at : at + weight.shape[0]] = lax.dot_general(
                hidden_ref[j * tall : (j + 1) * tall, :],
                weight,
                (((1,), (1,)), ((), ())),
                preferred_element_type=F32,
            ).astype(BF16)
            at += weight.shape[0]


def merge_kernel(n_tp, *refs):
    in_refs, out_refs = refs[:n_tp], refs[n_tp:]
    share = out_refs[0].shape[0]
    for k, out_ref in enumerate(out_refs):
        rows = slice(k * share, (k + 1) * share)
        total = in_refs[0][rows, :].astype(F32)
        for in_ref in in_refs[1:]:
            total = total + in_ref[rows, :].astype(F32)
        out_ref[...] = total.astype(BF16)


def last_kernel(groups, width, planes, mid_ref, *refs):
    part_refs, out_ref, total_ref = refs[:-2], refs[-2], refs[-1]
    ring_at = ring_place(lax.div(lax.axis_index("sp"), width), planes)
    columns = total_ref.shape[-1]
    for g, spans in enumerate(groups):
        at = 0
        for i, offset, length in spans:
            plane = ring_plane(lax.rem(ring_at - i + planes, planes), planes)
            total = part_refs[g * width][:, at : at + length].astype(F32)
            for part_ref in part_refs[g * width + 1 : (g + 1) * width]:
                total = total + part_ref[:, at : at + length].astype(F32)
            total_ref[plane, :, offset : offset + length] = total
            at += length
    for plane in range(planes):
        cols = slice(plane * columns, (plane + 1) * columns)
        out_ref[:, cols] = (mid_ref[:, cols].astype(F32) + total_ref[plane]).astype(BF16)


def body(
    queries,
    keys,
    values,
    documents,
    query_gain,
    key_gain,
    out_weight,
    residual,
    norm_gain,
    up_weight,
    down_weight,
):
    n_sp, n_tp = lax.axis_size("sp"), lax.axis_size("tp")
    tokens, heads, head = queries.shape
    width_d = residual.shape[1]
    rows_w, columns = up_weight.shape
    width = plane_width(n_sp, columns)
    planes = n_sp // width
    units = columns // width
    share = tokens // n_tp
    halves = 2 if width > 1 else 1
    each = width // halves
    order = ring_order(planes)
    place = lax.rem(lax.axis_index("sp"), width)

    def beside(x, k):
        return lax.ppermute(x, "sp", [(s, s // width * width + (s % width ^ k)) for s in range(n_sp)])

    def along(x, k=1):
        pairs = []
        for at, plane in enumerate(order):
            to = order[(at + k) % planes]
            pairs += [(plane * width + b, to * width + b) for b in range(width)]
        return lax.ppermute(x, "sp", pairs)

    def across(x, j):
        return lax.ppermute(x, "tp", [(t, (t + j) % n_tp) for t in range(n_tp)])

    def column_block(w, k):
        return lax.dynamic_slice_in_dim(w, jnp.bitwise_xor(place, k) * units, units, 1)

    up_in = [column_block(up_weight, k) for k in range(width)]
    up_in = up_in[:1] + [beside(up_in[k], k) for k in range(1, width)]
    down_in = [column_block(down_weight, k) for k in range(width)]
    down_in = down_in[:1] + [beside(down_in[k], k) for k in range(1, width)]

    kv_index = lax.axis_index("tp") * heads // (QUERY_HEADS // keys.shape[1])
    own_keys = lax.dynamic_index_in_dim(keys, kv_index, 1, keepdims=False)
    own_values = lax.dynamic_index_in_dim(values, kv_index, 1, keepdims=False)
    kv = call(
        key_kernel,
        shape((tokens + DOC_ROWS, 2 * head)),
        (own_keys, own_values, documents.reshape(1, tokens), key_gain.reshape(1, head)),
        name="key",
        flops=10**8,
    )
    kv = jnp.concatenate([kv] + [along(kv, k) for k in range(1, planes)], 0)
    kvs = [kv] + [beside(kv, k) for k in range(1, width)]
    query = call(
        functools.partial(query_kernel, heads),
        shape((tokens, heads * head)),
        (queries.reshape(tokens, heads * head), query_gain.reshape(1, head)),
        name="query",
        flops=10**8,
    )

    def stack(parts):
        return jnp.stack(parts, 0)

    ups = [[stack(up_in[h * each : (h + 1) * each]) for h in range(halves)]]
    downs = [
        call(
            functools.partial(sort_kernel, width),
            [shape((each, rows_w, units)) for _ in range(halves)],
            down_in,
            name="sort",
        )
    ]
    for _ in range(planes - 1):
        ups.append([along(x) for x in ups[-1]])
        downs.append([along(x) for x in downs[-1]])

    parts = call(
        functools.partial(attend_kernel, heads, n_tp, planes),
        [shape((share, width_d)) for _ in range(n_tp)],
        (query, documents.reshape(tokens, 1), out_weight, *kvs),
        scratch=[
            pltpu.VMEM((heads, tokens, 1), F32),
            pltpu.VMEM((heads, tokens, 1), F32),
            pltpu.VMEM((heads, tokens, head), F32),
            pltpu.VMEM((tokens, heads * head), BF16),
        ],
        name="attend",
        flops=10**9,
    )
    parts = parts[:1] + [across(parts[j], j) for j in range(1, n_tp)]
    mid, normed = call(
        functools.partial(mid_kernel, n_tp),
        [shape((share, width_d))] * 2,
        (residual, norm_gain.reshape(1, width_d), *parts),
        name="mid",
        flops=10**8,
    )

    normed = [normed] + [beside(normed, k) for k in range(1, width)]
    pieces = list(normed)
    for j in range(1, n_tp):
        pieces += [across(x, j) for x in normed]
    hidden = call(
        functools.partial(up_kernel, len(pieces), planes, width),
        shape((len(pieces) * share, units)),
        (*pieces, *[x for pair in ups for x in pair]),
        scratch=[
            pltpu.VMEM((len(pieces) * share, width_d), BF16),
            pltpu.VMEM((n_sp, rows_w, units), BF16),
        ],
        name="up",
        flops=10**9,
    )

    half_cols, plane_cols = each * rows_w, width * rows_w
    if planes > 2 and halves > 1:
        groups = [
            [(i, 0, plane_cols) for i in range(planes - 2)],
            [(planes - 2, 0, plane_cols)],
        ] + [[(planes - 1, h * half_cols, half_cols)] for h in range(halves)]
    else:
        groups = [[(i, 0, plane_cols)] for i in range(planes)]
    sums = []
    for spans in groups:
        chunk = []
        for i, offset, length in spans:
            chunk += downs[i][offset // half_cols : (offset + length) // half_cols]
        cols = sum(length for _, _, length in spans)
        out = call(
            functools.partial(down_kernel, n_tp),
            [shape((width * share, cols)) for _ in range(n_tp)],
            (hidden, *chunk),
            name="down",
            flops=cols * 10**5,
        )
        out = out[:1] + [across(out[j], n_tp - j) for j in range(1, n_tp)]
        out = call(
            functools.partial(merge_kernel, n_tp),
            [shape((share, cols)) for _ in range(width)],
            out,
            name="merge",
        )
        sums += out[:1] + [beside(out[k], k) for k in range(1, width)]
    return call(
        functools.partial(last_kernel, groups, width, planes),
        shape((share, width_d)),
        (mid, *sums),
        scratch=[pltpu.VMEM((planes, share, plane_cols), F32)],
        name="last",
    )


def solution(mesh):
    in_specs = (
        P("sp", "tp", None),
        P("sp", None, None),
        P("sp", None, None),
        P("sp"),
        P(),
        P(),
        P("tp", None),
        P("sp", None),
        P(),
        P("sp", "tp"),
        P("sp", "tp"),
    )
    out_specs = P(("sp", "tp"), None)
    return jax.shard_map(body, mesh=mesh, in_specs=in_specs, out_specs=out_specs, check_vma=False)
```

```python
import functools

import jax
import jax.numpy as jnp
from jax import lax
from jax.experimental import pallas as pl
from jax.experimental.pallas import tpu as pltpu
from jax.sharding import PartitionSpec as P


QUERY_HEADS = 8
GRID = 64
EPS = 1e-06
THETA = 10000.0
LANES = 128
DOC_ROWS = 16
LOG2E = 1.4426950408889634
VMEM = pl.BlockSpec(memory_space=pltpu.VMEM)
BF16, F32 = jnp.bfloat16, jnp.float32


def call(kernel, outs, args, scratch=(), flops=0):
    run = pl.pallas_call(
        kernel,
        out_shape=outs,
        in_specs=[VMEM] * len(args),
        out_specs=jax.tree.map(lambda _: VMEM, outs),
        scratch_shapes=list(scratch),
        compiler_params=pltpu.CompilerParams(vmem_limit_bytes=48 * 1024 * 1024),
        cost_estimate=pl.CostEstimate(flops=flops, bytes_accessed=0, transcendentals=0),
    )
    result = run(*args)
    return list(result) if isinstance(outs, list) else result


def shape(dims, dtype=BF16):
    return jax.ShapeDtypeStruct(dims, dtype)


def ring_place(plane, planes):
    return jnp.where(plane % 2 == 1, (plane + 1) // 2, jnp.where(plane == 0, 0, planes - plane // 2))


def ring_plane(at, planes):
    return jnp.where(at <= planes // 2, jnp.maximum(2 * at - 1, 0), 2 * (planes - at))


def ring_order(planes):
    return [0] + list(range(1, planes, 2)) + list(range((planes - 1) // 2 * 2, 0, -2))


def plane_width(n_sp, columns):
    width = 1
    while (4 * width * width <= n_sp) and n_sp % (2 * width) == 0 and columns % (2 * width * LANES) == 0:
        width *= 2
    return width


def rope_tables(base, rows, head):
    quarter = head // 4
    lane = lax.broadcasted_iota(jnp.int32, (rows, head), 1)
    position = base + lax.broadcasted_iota(jnp.int32, (rows, head), 0)
    where = jnp.where(lane < 2 * quarter, position // GRID, position % GRID).astype(F32)
    step = (lane % quarter).astype(F32) / quarter
    angle = where * jnp.exp(step * (-jnp.log(jnp.float32(THETA))))
    first = lane % (2 * quarter) < quarter
    return jnp.cos(angle), jnp.sin(angle), first


def norm_rope(block, gain, tables):
    cosine, sine, first = tables
    head = block.shape[-1]
    block = block.astype(F32)
    block = block * lax.rsqrt(jnp.mean(block * block, axis=-1, keepdims=True) + EPS) * gain
    turned = jnp.where(first, -pltpu.roll(block, head - head // 4, 1), pltpu.roll(block, head // 4, 1))
    return (block * cosine + turned * sine).astype(BF16)


def key_kernel(key_ref, value_ref, doc_ref, gain_ref, out_ref):
    rows, head = key_ref.shape
    tables = rope_tables(lax.axis_index("sp") * rows, rows, head)
    key = norm_rope(key_ref[...], gain_ref[...], tables)
    for n in range(rows // head):
        out_ref[0:head, n * head : (n + 1) * head] = key[n * head : (n + 1) * head, :]
    out_ref[head : 2 * head, :] = value_ref[...].astype(F32).T.astype(BF16)
    docs = doc_ref[...].astype(F32)
    out_ref[2 * head :, :] = jnp.broadcast_to(docs, (DOC_ROWS, rows)).astype(BF16)


def query_kernel(heads, query_ref, gain_ref, out_ref):
    rows = query_ref.shape[0]
    head = query_ref.shape[1] // heads
    tables = rope_tables(lax.axis_index("sp") * rows, rows, head)
    for h in range(heads):
        query = norm_rope(query_ref[:, h * head : (h + 1) * head], gain_ref[...], tables)
        out_ref[:, h * rows : (h + 1) * rows] = query.astype(F32).T.astype(BF16)


def attend_kernel(heads, n_tp, blocks, begins, ends, query_ref, doc_ref, *refs):
    refs = list(refs)
    if ends:
        out_weight_ref = refs.pop(0)
    states = [] if begins else [refs.pop(0) for _ in range(3)]
    flag_ref, attn_ref = refs.pop(-2), refs.pop(-1)
    if ends:
        work_refs = [refs.pop(-1) for _ in range(3)][::-1]
        out_refs = [refs.pop(-1) for _ in range(n_tp)][::-1]
    else:
        work_refs = [refs.pop(-1) for _ in range(3)][::-1]
    kv_refs = refs
    peak_ref, denom_ref, sum_ref = work_refs
    head = query_ref.shape[0]
    rows = query_ref.shape[1] // heads
    height = 2 * head + DOC_ROWS
    scale = head ** (-0.5) * LOG2E
    if begins:
        peak_ref[...] = jnp.full(peak_ref.shape, -1e29, F32)
        sum_ref[...] = jnp.zeros(sum_ref.shape, F32)
        denom_ref[...] = jnp.zeros(denom_ref.shape, F32)
    else:
        for work_ref, state_ref in zip(work_refs, states):
            work_ref[...] = state_ref[...]
    own = doc_ref[...].astype(F32)
    first_doc, last_doc = jnp.min(own), jnp.max(own)
    for n, kv_ref in enumerate(kv_refs):
        for i in range(blocks):
            docs = kv_ref[i * height + 2 * head : (i + 1) * height, :].astype(F32)
            touches = jnp.logical_and(jnp.min(docs) <= last_doc, jnp.max(docs) >= first_doc)
            flag_ref[n * blocks + i] = touches.astype(jnp.int32)

    def block(kv_ref, at):
        docs = kv_ref[pl.ds(at + 2 * head, DOC_ROWS), :].astype(F32)[0:8, :]
        allowed = docs.T[:, 0:1] == own
        keys = jnp.concatenate(
            [kv_ref[pl.ds(at, head), n * head : (n + 1) * head] for n in range(rows // head)], 0
        )
        vals = kv_ref[pl.ds(at + head, head), :]
        for h in range(heads):
            s = jnp.dot(
                keys, query_ref[:, h * rows : (h + 1) * rows], preferred_element_type=F32
            )
            s = jnp.where(allowed, s * scale, -1e30)
            old = peak_ref[h]
            new = jnp.maximum(old, jnp.max(s, axis=0, keepdims=True))
            peak_ref[h] = new
            p = jnp.exp2(s - new)
            keep = jnp.exp2(old - new)
            denom_ref[h] = denom_ref[h] * keep + jnp.sum(p, axis=0, keepdims=True)
            sum_ref[h] = sum_ref[h] * keep + jnp.dot(
                vals, p.astype(BF16), preferred_element_type=F32
            )

    for n, kv_ref in enumerate(kv_refs):

        @pl.loop(0, blocks)
        def _(i):
            @pl.when(flag_ref[n * blocks + i] == 1)
            def _():
                block(kv_ref, pl.multiple_of(i * height, DOC_ROWS))

    if not ends:
        return
    for h in range(heads):
        attn = (sum_ref[h] / denom_ref[h]).T
        attn_ref[:, h * head : (h + 1) * head] = attn.astype(BF16)
    share = rows // n_tp
    for j, out_ref in enumerate(out_refs):
        at = lax.rem(lax.axis_index("tp") + j, n_tp) * share
        out_ref[...] = jnp.dot(
            attn_ref[pl.ds(pl.multiple_of(at, share), share), :],
            out_weight_ref[...],
            preferred_element_type=F32,
        ).astype(BF16)


def cut_kernel(width, weight_ref, *out_refs):
    place = lax.rem(lax.axis_index("sp"), width)
    units = out_refs[0].shape[-1]
    for k, out_ref in enumerate(out_refs):
        at = jnp.bitwise_xor(place, k) * units
        out_ref[...] = weight_ref[:, pl.ds(pl.multiple_of(at, LANES), units)]


def mid_kernel(n_tp, residual_ref, gain_ref, *refs):
    part_refs, (mid_ref, normed_ref) = refs[:n_tp], refs[n_tp:]
    share = mid_ref.shape[0]
    at = pl.multiple_of(lax.axis_index("tp") * share, share)
    branch = part_refs[0][...].astype(F32)
    for part_ref in part_refs[1:]:
        branch = branch + part_ref[...].astype(F32)
    mid = (residual_ref[pl.ds(at, share), :].astype(F32) + branch).astype(BF16)
    mid_ref[...] = mid
    mid = mid.astype(F32)
    scale = lax.rsqrt(jnp.mean(mid * mid, axis=-1, keepdims=True) + EPS)
    normed_ref[...] = (mid * scale * gain_ref[...]).astype(BF16)


def up_kernel(pieces, planes, width, *refs):
    piece_refs, w_refs = refs[:pieces], refs[pieces:-3]
    out_ref, rows_ref, weight_ref = refs[-3:]
    share = piece_refs[0].shape[0]
    place = lax.rem(lax.axis_index("sp"), width)
    ring_at = ring_place(lax.div(lax.axis_index("sp"), width), planes)
    for n, piece_ref in enumerate(piece_refs):
        rows_ref[n * share : (n + 1) * share, :] = piece_ref[...]
    per_plane = len(w_refs) // planes
    for i in range(planes):
        plane = ring_plane(lax.rem(ring_at - i + planes, planes), planes)
        k = 0
        for w_ref in w_refs[i * per_plane : (i + 1) * per_plane]:
            for n in range(w_ref.shape[0]):
                weight_ref[plane * width + jnp.bitwise_xor(place, k)] = w_ref[n]
                k += 1
    weight = weight_ref[...].reshape(-1, weight_ref.shape[-1])
    tall = min(512, rows_ref.shape[0])

    @pl.loop(0, rows_ref.shape[0] // tall)
    def _(n):
        at = pl.ds(pl.multiple_of(n * tall, tall), tall)
        raised = jnp.dot(rows_ref[at, :], weight, preferred_element_type=F32)
        raised = jnp.maximum(raised, 0.0)
        out_ref[at, :] = (raised * raised).astype(BF16)


def sort_kernel(width, *refs):
    in_refs, out_refs = refs[:width], refs[width:]
    place = lax.rem(lax.axis_index("sp"), width)
    each = width // len(out_refs)
    for k, in_ref in enumerate(in_refs):
        to = jnp.bitwise_xor(place, k)
        for h, out_ref in enumerate(out_refs):

            @pl.when(lax.div(to, each) == h)
            def _():
                out_ref[lax.rem(to, each)] = in_ref[...]


def down_kernel(n_tp, hidden_ref, *refs):
    w_refs, out_refs = refs[:-n_tp], refs[-n_tp:]
    tall = out_refs[0].shape[0]
    for j, out_ref in enumerate(out_refs):
        at = 0
        for w_ref in w_refs:
            weight = w_ref[...].reshape(-1, w_ref.shape[-1])
            out_ref[:, at : at + weight.shape[0]] = lax.dot_general(
                hidden_ref[j * tall : (j + 1) * tall, :],
                weight,
                (((1,), (1,)), ((), ())),
                preferred_element_type=F32,
            ).astype(BF16)
            at += weight.shape[0]


def merge_kernel(n_tp, *refs):
    in_refs, out_refs = refs[:n_tp], refs[n_tp:]
    share = out_refs[0].shape[0]
    for k, out_ref in enumerate(out_refs):
        rows = slice(k * share, (k + 1) * share)
        total = in_refs[0][rows, :].astype(F32)
        for in_ref in in_refs[1:]:
            total = total + in_ref[rows, :].astype(F32)
        out_ref[...] = total.astype(BF16)


def last_kernel(groups, width, planes, mid_ref, *refs):
    part_refs, out_ref, total_ref = refs[:-2], refs[-2], refs[-1]
    ring_at = ring_place(lax.div(lax.axis_index("sp"), width), planes)
    columns = total_ref.shape[-1]
    for g, spans in enumerate(groups):
        at = 0
        for i, offset, length in spans:
            plane = ring_plane(lax.rem(ring_at - i + planes, planes), planes)
            total = part_refs[g * width][:, at : at + length].astype(F32)
            for part_ref in part_refs[g * width + 1 : (g + 1) * width]:
                total = total + part_ref[:, at : at + length].astype(F32)
            total_ref[plane, :, offset : offset + length] = total
            at += length
    for plane in range(planes):
        cols = slice(plane * columns, (plane + 1) * columns)
        out_ref[:, cols] = (mid_ref[:, cols].astype(F32) + total_ref[plane]).astype(BF16)


def body(
    queries,
    keys,
    values,
    documents,
    query_gain,
    key_gain,
    out_weight,
    residual,
    norm_gain,
    up_weight,
    down_weight,
):
    n_sp, n_tp = lax.axis_size("sp"), lax.axis_size("tp")
    tokens, heads, head = queries.shape
    width_d = residual.shape[1]
    rows_w, columns = up_weight.shape
    width = plane_width(n_sp, columns)
    planes = n_sp // width
    units = columns // width
    share = tokens // n_tp
    halves = 2 if width > 1 else 1
    each = width // halves
    order = ring_order(planes)
    place = lax.rem(lax.axis_index("sp"), width)

    def beside(x, k):
        return lax.ppermute(
            x, "sp", [(s, s // width * width + (s % width ^ k)) for s in range(n_sp)]
        )

    def along(x, k):
        pairs = []
        for at, plane in enumerate(order):
            to = order[(at + k) % planes]
            pairs += [(plane * width + b, to * width + b) for b in range(width)]
        return lax.ppermute(x, "sp", pairs)

    def across(x, j):
        return lax.ppermute(x, "tp", [(t, (t + j) % n_tp) for t in range(n_tp)])

    def exchange(w):
        cut = call(
            functools.partial(cut_kernel, width),
            [shape((rows_w, units)) for _ in range(width)],
            (w,),
        )
        return cut[:1] + [beside(cut[k], k) for k in range(1, width)]

    up_in = exchange(up_weight)
    down_in = exchange(down_weight)

    kv_index = lax.axis_index("tp") * heads // (QUERY_HEADS // keys.shape[1])
    own_keys = lax.dynamic_index_in_dim(keys, kv_index, 1, keepdims=False)
    own_values = lax.dynamic_index_in_dim(values, kv_index, 1, keepdims=False)
    docs = documents.reshape(1, tokens)
    kv = call(
        key_kernel,
        shape((2 * head + DOC_ROWS, tokens)),
        (own_keys, own_values, docs, key_gain.reshape(1, head)),
        flops=10**8,
    )
    kv = jnp.concatenate([kv] + [along(kv, k) for k in range(1, planes)], 0)
    kvs = [kv] + [beside(kv, k) for k in range(1, width)]
    query = call(
        functools.partial(query_kernel, heads),
        shape((head, heads * tokens)),
        (queries.reshape(tokens, heads * head), query_gain.reshape(1, head)),
        flops=10**8,
    )

    ups = [[jnp.stack(up_in[h * each : (h + 1) * each], 0) for h in range(halves)]]
    downs = [
        call(
            functools.partial(sort_kernel, width),
            [shape((each, rows_w, units)) for _ in range(halves)],
            down_in,
        )
    ]
    for _ in range(1, planes):
        ups.append([along(x, 1) for x in ups[-1]])
        downs.append([along(x, 1) for x in downs[-1]])

    state_dims = [(heads, 1, tokens), (heads, 1, tokens), (heads, head, tokens)]
    stages = [kvs[:1], kvs[1:-1], kvs[-1:]] if width > 2 else [kvs]
    state = []
    for n, stage in enumerate(stages):
        begins, ends = n == 0, n == len(stages) - 1
        state = call(
            functools.partial(attend_kernel, heads, n_tp, planes, begins, ends),
            [shape((share, width_d))] * n_tp if ends else [shape(d, F32) for d in state_dims],
            (query, docs, *([out_weight] if ends else []), *state, *stage),
            scratch=([pltpu.VMEM(d, F32) for d in state_dims] if ends else [])
            + [
                pltpu.SMEM((len(stage) * planes,), jnp.int32),
                pltpu.VMEM((tokens, heads * head), BF16),
            ],
            flops=10**9,
        )
    parts = state
    parts = parts[:1] + [across(parts[j], j) for j in range(1, n_tp)]
    mid, normed = call(
        functools.partial(mid_kernel, n_tp),
        [shape((share, width_d))] * 2,
        (residual, norm_gain.reshape(1, width_d), *parts),
        flops=10**8,
    )

    normed = [normed] + [beside(normed, k) for k in range(1, width)]
    pieces = list(normed)
    for j in range(1, n_tp):
        pieces += [across(x, j) for x in normed]
    hidden = call(
        functools.partial(up_kernel, len(pieces), planes, width),
        shape((len(pieces) * share, units)),
        (*pieces, *[x for pair in ups for x in pair]),
        scratch=[
            pltpu.VMEM((len(pieces) * share, width_d), BF16),
            pltpu.VMEM((n_sp, rows_w, units), BF16),
        ],
        flops=10**9,
    )

    half_cols, plane_cols = each * rows_w, width * rows_w
    groups = token_groups(planes, halves, half_cols)
    sums = []
    for spans in groups:
        chunk = []
        for i, offset, length in spans:
            chunk += downs[i][offset // half_cols : (offset + length) // half_cols]
        cols = sum(length for _, _, length in spans)
        out = call(
            functools.partial(down_kernel, n_tp),
            [shape((width * share, cols)) for _ in range(n_tp)],
            (hidden, *chunk),
            flops=cols * 10**5,
        )
        out = out[:1] + [across(out[j], n_tp - j) for j in range(1, n_tp)]
        out = call(
            functools.partial(merge_kernel, n_tp), [shape((share, cols)) for _ in range(width)], out
        )
        sums += out[:1] + [beside(out[k], k) for k in range(1, width)]
    return call(
        functools.partial(last_kernel, groups, width, planes),
        shape((share, width_d)),
        (mid, *sums),
        scratch=[pltpu.VMEM((planes, share, plane_cols), F32)],
    )


def token_groups(planes, halves, half_cols):
    plane_cols = halves * half_cols
    if planes > 2 and halves > 1:
        return [
            [(i, 0, plane_cols) for i in range(planes - 2)],
            [(planes - 2, 0, plane_cols)],
        ] + [[(planes - 1, h * half_cols, half_cols)] for h in range(halves)]
    return [[(i, 0, plane_cols)] for i in range(planes)]


def solution(mesh):
    in_specs = (
        P("sp", "tp", None),
        P("sp", None, None),
        P("sp", None, None),
        P("sp"),
        P(),
        P(),
        P("tp", None),
        P("sp", None),
        P(),
        P("sp", "tp"),
        P("sp", "tp"),
    )
    out_specs = P(("sp", "tp"), None)
    return jax.shard_map(body, mesh=mesh, in_specs=in_specs, out_specs=out_specs, check_vma=False)
```
